512 devices in a mesh: sp: 128 (over z, y, core), tp: 4 (over x).
Axes of the slice: x: 4, y: 8, z: 8, core: 2. Of those that a mesh axis runs over, the one named last changes fastest.
Arguments:
- tokens: bfloat16 [16384, 2048], P(('sp', 'tp')), may hold values from -6 to 6
- norm_gain: float32 [2048], replicated, may hold values from 0.1 to 1.9
- w_filter_b: bfloat16 [2048, 1024], P('sp', 'tp'), may hold values from -0.125 to 0.125
- w_filter_c: bfloat16 [2048, 1024], P('sp', 'tp'), may hold values from -0.125 to 0.125
- w_filter_v: bfloat16 [2048, 1024], P('sp', 'tp'), may hold values from -0.125 to 0.125
- filter_taps: float32 [3, 1024], P(None, 'tp'), may hold values from -3.5 to 3.5
- w_query: bfloat16 [2048, 1024], P('sp', 'tp'), may hold values from -0.125 to 0.125
- retention_gate_matrix: bfloat16 [2048, 1024], P('sp', 'tp'), may hold values from -0.125 to 0.125
- w_input: bfloat16 [2048, 1024], P('sp', 'tp'), may hold values from -0.125 to 0.125
- forget_gap: float32 [1024], P('tp'), may hold values from 0 to 0.12
- additive_fade_log: float32 [16384, 1024], P('sp', 'tp'), may hold values from -1.1 to 0
- head_gain: float32 [128], replicated, may hold values from 0.1 to 1.9
- initial_state: float32 [8, 128, 128], P('tp'), may hold values from -0.013671875 to 0.013671875
- w_out_filter: bfloat16 [1024, 2048], P('tp'), may hold values from -0.125 to 0.125
- w_out_rec: bfloat16 [1024, 2048], P('tp'), may hold values from -0.125 to 0.125
Outputs:
- mixed: bfloat16 [16384, 2048], P(('sp', 'tp'))
The draws below stay inside these ranges and needn't reach their ends.
All inputs are finite; a program needn't handle non-finite values.
Results may differ from the reference program's by a relative error of at most 0.03.
Values may be sent and summed in bfloat16 or wider, within the bound.
No kernel may reach another device: no remote copies, remote signals or barrier semaphores. Data moves between devices by JAX's collectives and lax.ppermute only.
A program may use at most 64 MiB of HBM per device.

```python
import math
import jax
import jax.numpy as jnp
from jax import lax

D = 2048
CONV = 1024
HEADS = 8
HEAD_DIM = 128
SPAN = 64
TAPS = 3
TOK_DEV = 128
FEATURE_SPAN = 1024
SEQUENCE_SIZE = 16384
N_TP = 4


def draw_forget_gap(key, part):
    order_key, fast_key, slow_key = jax.random.split(jax.random.fold_in(key, 11), 3)
    slow_count = HEADS // 2
    ranking = jax.random.permutation(order_key, HEADS)
    slow_head = ranking < slow_count
    fast_gap = jnp.exp(jax.random.uniform(fast_key, (HEADS, HEAD_DIM), jnp.float32, math.log(0.04), math.log(0.12)))
    slow_gap = jnp.exp(jax.random.uniform(slow_key, (HEADS, HEAD_DIM), jnp.float32, math.log(0.2), math.log(0.6))) / SEQUENCE_SIZE
    return jnp.where(slow_head[:, None], slow_gap, fast_gap).reshape(HEADS * HEAD_DIM)


def draw_additive_fade_log(key, part):
    rate_key, factor_key, spot_key, loss_key = jax.random.split(jax.random.fold_in(key, 23), 4)
    low_factor, high_factor = (0.5, 2.0)
    base_rate = jnp.exp(jax.random.uniform(rate_key, (FEATURE_SPAN,), jnp.float32, math.log(0.1), math.log(0.4))) / SEQUENCE_SIZE
    segments = SEQUENCE_SIZE // TOK_DEV
    factor = jnp.exp(jax.random.uniform(factor_key, (segments, 1, FEATURE_SPAN), jnp.float32, math.log(low_factor), math.log(high_factor)))
    settled_memory = -(base_rate[None, None, :] * factor) * jnp.ones((1, TOK_DEV, 1), jnp.float32)
    spot_rows = jax.random.randint(spot_key, (3,), 0, SEQUENCE_SIZE)
    objective_entries = jax.random.uniform(loss_key, (3,), jnp.float32, 0.2, 0.4)
    indexed_catalog = (jnp.arange(SEQUENCE_SIZE)[:, None] == spot_rows[None, :]).astype(jnp.float32)
    packet_bundles = jnp.sum(indexed_catalog * jnp.log1p(-objective_entries)[None, :], axis=1)
    return settled_memory.reshape(SEQUENCE_SIZE, FEATURE_SPAN) + packet_bundles[:, None]


def shard_levels(stream_key, shape, shards, least, top_value):
    gain = 1.0
    for position, blocks in shards:
        heights = jax.random.uniform(jax.random.fold_in(jax.random.fold_in(stream_key, 6), position), (blocks,), jnp.float32, least / len(shards), top_value / len(shards))
        gain = gain * jnp.repeat(jnp.exp(heights), shape[position] // blocks).reshape((-1,) + (1,) * (len(shape) - 1 - position))
    return gain


def bell_draw(rng, shape, scale, most, cuts=(), held_as=jnp.bfloat16):
    gain = shard_levels(rng, shape, cuts, -0.22, 0.18) if cuts else 1.0
    array = jax.random.normal(rng, shape, jnp.float32) * scale * gain
    return jnp.minimum(jnp.maximum(array, -most), most).astype(held_as)


def setup_inputs(seed: int = 0) -> dict:
    arg_keys = jax.random.split(jax.random.key(seed), 16)
    return {
        "tokens": bell_draw(arg_keys[0], (SEQUENCE_SIZE, D), 1.0, 6.0, ((0, 512),)),
        "norm_gain": jnp.clip(1.0 + 0.18 * jax.random.normal(arg_keys[1], (D,), jnp.float32), 0.1, 1.9),
        "w_filter_b": bell_draw(arg_keys[2], (D, CONV), D ** -0.5, 0.125, ((0, 128), (1, 4))),
        "w_filter_c": bell_draw(arg_keys[3], (D, CONV), D ** -0.5, 0.125, ((0, 128), (1, 4))),
        "w_filter_v": bell_draw(arg_keys[4], (D, CONV), D ** -0.5, 0.125, ((0, 128), (1, 4))),
        "filter_taps": bell_draw(arg_keys[5], (TAPS, CONV), TAPS ** -0.5, 3.5, ((1, 4),), jnp.float32),
        "w_query": bell_draw(arg_keys[6], (D, FEATURE_SPAN), D ** -0.5, 0.125, ((0, 128), (1, 4))),
        "retention_gate_matrix": bell_draw(arg_keys[7], (D, FEATURE_SPAN), D ** -0.5, 0.125, ((0, 128), (1, 4))),
        "w_input": bell_draw(arg_keys[8], (D, FEATURE_SPAN), D ** -0.5, 0.125, ((0, 128), (1, 4))),
        "forget_gap": draw_forget_gap(jax.random.fold_in(arg_keys[15], 71), 0),
        "additive_fade_log": draw_additive_fade_log(jax.random.fold_in(arg_keys[15], 71), 0),
        "head_gain": jnp.clip(1.0 + 0.18 * jax.random.normal(arg_keys[11], (HEAD_DIM,), jnp.float32), 0.1, 1.9),
        "initial_state": bell_draw(arg_keys[12], (HEADS, HEAD_DIM, HEAD_DIM), (0.3 * SEQUENCE_SIZE ** -0.5), 0.013671875, ((0, 4),), jnp.float32),
        "w_out_filter": bell_draw(arg_keys[13], (CONV, D), (CONV + FEATURE_SPAN) ** -0.5, 0.125, ((0, 4),)),
        "w_out_rec": bell_draw(arg_keys[14], (FEATURE_SPAN, D), (CONV + FEATURE_SPAN) ** -0.5, 0.125, ((0, 4),)),
    }


epsilon = 1e-06
highest_precision = lax.Precision.HIGHEST

def block_step(carried_state, inputs):
    block_query, block_key, block_value_rows, block_decay = inputs
    causal = jnp.tril(jnp.ones((SPAN, SPAN), dtype=bool))
    running = jnp.cumsum(block_decay, axis=0)
    scaled_query = block_query * jnp.exp(running)
    key_scaled = block_key * jnp.exp(-running)
    scores = jnp.einsum('thk,shk->hts', scaled_query, key_scaled, precision=highest_precision)
    scores = jnp.where(causal[None], scores, 0.0)
    final_result = jnp.einsum('hts,shv->thv', scores, block_value_rows, precision=highest_precision)
    final_result = final_result + jnp.einsum('oql,qlz->oqz', scaled_query, carried_state, precision=highest_precision)
    final_state = running[-1]
    key_remainder = block_key * jnp.exp(final_state[None] - running)
    updated_state = jnp.exp(final_state)[:, :, None] * carried_state + jnp.einsum('dri,drz->riz', key_remainder, block_value_rows, precision=highest_precision)
    return (updated_state, final_result)

def reference(tokens, norm_gain, w_filter_b, w_filter_c, w_filter_v, filter_taps, w_query, retention_gate_matrix, w_input, forget_gap, additive_fade_log, head_gain, initial_state, w_out_filter, w_out_rec):
    widened = tokens.astype(jnp.float32)
    normed = (widened * lax.rsqrt(lax.optimization_barrier(jnp.mean(widened * widened, axis=-1, keepdims=True)) + epsilon) * norm_gain).astype(jnp.bfloat16)

    def project(weight):
        return jnp.dot(normed, weight, preferred_element_type=jnp.float32).astype(jnp.bfloat16)
    gate_out = project(w_filter_b)
    product = project(w_filter_c).astype(jnp.float32) * project(w_filter_v).astype(jnp.float32)
    padded = jnp.concatenate([jnp.zeros((TAPS - 1, CONV), jnp.float32), product], axis=0)
    filtered = jnp.zeros_like(product)
    for offset in range(TAPS):
        filtered = filtered + filter_taps[offset] * padded[offset:offset + SEQUENCE_SIZE]
    filter_out = (gate_out.astype(jnp.float32) * filtered).astype(jnp.bfloat16)
    queries = project(w_query).astype(jnp.float32)
    forget_logit = project(retention_gate_matrix).astype(jnp.float32)
    input_value = project(w_input).astype(jnp.float32)
    key_rate = forget_gap * jax.nn.sigmoid(-forget_logit)
    log_decay = jnp.log1p(-key_rate) + additive_fade_log
    value_in = jax.nn.silu(input_value)

    def heads_blocks(flat_rows):
        return flat_rows.reshape(SEQUENCE_SIZE // SPAN, SPAN, HEADS, HEAD_DIM)
    ignored_state, unmixed_output = lax.scan(block_step, initial_state, (heads_blocks(queries), heads_blocks(key_rate), heads_blocks(value_in), heads_blocks(log_decay)))
    unmixed_output = unmixed_output.reshape(SEQUENCE_SIZE, HEADS, HEAD_DIM)
    rec_out = (unmixed_output * lax.rsqrt(lax.optimization_barrier(jnp.mean(unmixed_output * unmixed_output, axis=-1, keepdims=True)) + epsilon) * head_gain).astype(jnp.bfloat16).reshape(SEQUENCE_SIZE, FEATURE_SPAN)
    filter_group = CONV // N_TP
    recur_group = FEATURE_SPAN // N_TP
    summed = jnp.zeros((SEQUENCE_SIZE, D), jnp.float32)
    for member in range(N_TP):
        filter_part = filter_out[:, member * filter_group:(member + 1) * filter_group]
        recur_part = rec_out[:, member * recur_group:(member + 1) * recur_group]
        partial_value = jnp.dot(filter_part, w_out_filter[member * filter_group:(member + 1) * filter_group], preferred_element_type=jnp.float32)
        partial_value = partial_value + jnp.dot(recur_part, w_out_rec[member * recur_group:(member + 1) * recur_group], preferred_element_type=jnp.float32)
        rounded = lax.optimization_barrier(partial_value.astype(jnp.bfloat16))
        summed = summed + rounded.astype(jnp.float32)
    return summed.astype(jnp.bfloat16)
```

```python
import jax
import jax.numpy as jnp
import numpy as np
from jax import lax
from jax.sharding import Mesh
from jax.sharding import PartitionSpec as P

HEAD_DIM = 128
SPAN = 64
TAPS = 3
HALO = 16
SP = ("sp_0", "sp_1", "sp_2")
SP_TP = ("sp_0", "sp_1", "sp_2", "tp")

epsilon = 1e-06
f32 = jnp.float32
bf16 = jnp.bfloat16


def exchanged(blocks, axis):
    return lax.all_to_all(blocks, axis, split_axis=0, concat_axis=0, tiled=True)


def sent_to_all(x, axis):
    return exchanged(jnp.broadcast_to(x, (lax.axis_size(axis), *x.shape)), axis)


def swapped(x, axis):
    return lax.ppermute(x, axis, [(0, 1), (1, 0)])


def shifted(block, axis):
    size = lax.axis_size(axis)
    return lax.ppermute(block, axis, [(i, i + 1) for i in range(size - 1)])


def running_sum(x):
    causal = jnp.tril(jnp.ones((x.shape[0], x.shape[0]), f32))
    return jnp.dot(causal, x, precision=lax.Precision.HIGHEST)


def rates(forget_logit, forget_gap, fade):
    key_rate = forget_gap * jax.nn.sigmoid(-forget_logit.astype(f32))
    return key_rate, jnp.log1p(-key_rate) + fade


def silu(v):
    return jax.nn.silu(v.astype(f32))


def state_of(key_rate, log_decay, value_in):
    running = running_sum(log_decay)
    remainder = (key_rate * jnp.exp(running[-1:] - running)).astype(bf16)
    state = jnp.einsum("tv,tk->vk", value_in.astype(bf16), remainder, preferred_element_type=f32)
    return running[-1], state


def pack(decay, state):
    high = lax.reduce_precision(decay, 8, 7)
    rest = decay - high
    low = lax.reduce_precision(rest, 8, 7)
    rows = jnp.stack([high, low, rest - low]).astype(bf16)
    return jnp.concatenate([state.astype(bf16), rows, jnp.zeros((13, HEAD_DIM), bf16)], axis=0)


def unpack(packed):
    decays = packed[:, HEAD_DIM : HEAD_DIM + 3].astype(f32).sum(axis=1)
    return decays, packed[:, :HEAD_DIM]


def weights_before(decays, position):
    size = decays.shape[0]
    place = jnp.arange(size)
    earlier = place < position
    kept = jnp.where(earlier[:, None], decays, 0.0)
    after = (place[None, :] > place[:, None]).astype(f32)
    since = jnp.sum(after[:, :, None] * kept[None], axis=1)
    return jnp.where(earlier[:, None], jnp.exp(since), 0.0), kept.sum(axis=0)


def weighted(weights, states):
    return jnp.sum(weights[:, None, :] * states.astype(f32), axis=0)


def body(
    tokens,
    norm_gain,
    w_filter_b,
    w_filter_c,
    w_filter_v,
    filter_taps,
    w_query,
    retention_gate_matrix,
    w_input,
    forget_gap,
    additive_fade_log,
    head_gain,
    initial_state,
    w_out_filter,
    w_out_rec,
):
    z, y, c = (lax.axis_index(a) for a in SP)
    own_rows = jnp.concatenate(
        [retention_gate_matrix, w_input, w_query, w_filter_b, w_filter_c, w_filter_v], axis=1
    )
    along_y = sent_to_all(own_rows, "sp_1").reshape(-1, own_rows.shape[1])
    weights = lax.all_gather(along_y, ("sp_0", "sp_2"), axis=0, tiled=True)

    gathered = sent_to_all(tokens, "tp").reshape(-1, tokens.shape[1])
    widened = gathered.astype(f32)
    normed = (
        widened
        * lax.rsqrt(jnp.mean(widened * widened, axis=-1, keepdims=True) + epsilon)
        * norm_gain
    ).astype(bf16)
    length, width = normed.shape
    order = np.arange(256).reshape(8, 2, 16).transpose(1, 0, 2).reshape(-1)
    swap = np.zeros((256, 256), np.float32)
    swap[order, np.arange(256)] = 1.0
    own = jnp.einsum(
        "tzk,kl->tzl",
        normed.reshape(length, 8, 256),
        jnp.asarray(swap, bf16),
        preferred_element_type=f32,
    ).astype(bf16).reshape(length, width)
    partner = swapped(own, "sp_2")
    halo = shifted(own[length - HALO :], SP)

    fade = additive_fade_log
    head = lambda a, k: lax.dynamic_slice_in_dim(a, k * HEAD_DIM, HEAD_DIM, axis=1)
    partner_fade = swapped(head(fade, 1 - c), "sp_2")

    chip = jnp.concatenate([own, partner], axis=0)
    chip_gates = jnp.dot(chip, weights[:, :512], preferred_element_type=f32).astype(bf16)
    forget_logit, input_value = chip_gates[:, :256], chip_gates[:, 256:]
    key_rate, log_decay = rates(forget_logit[:length], forget_gap, fade)
    value_in = silu(input_value[:length])
    gap_c = lax.dynamic_slice_in_dim(forget_gap, c * HEAD_DIM, HEAD_DIM)
    partner_rate, partner_decay = rates(head(forget_logit[length:], c), gap_c, partner_fade)
    partner_value = silu(head(input_value[length:], c))
    decay_own, state_own = state_of(head(key_rate, c), head(log_decay, c), head(value_in, c))
    decay_partner, state_partner = state_of(partner_rate, partner_decay, partner_value)
    first = c == 0
    decay_0, decay_1 = (
        jnp.where(first, decay_own, decay_partner),
        jnp.where(first, decay_partner, decay_own),
    )
    state_0, state_1 = (
        jnp.where(first, state_own, state_partner),
        jnp.where(first, state_partner, state_own),
    )
    state_chip = jnp.exp(decay_1)[None, :] * state_0 + state_1

    decays_y, states_y = unpack(sent_to_all(pack(decay_0 + decay_1, state_chip), "sp_1"))
    weights_row, decay_row = weights_before(decays_y, 8)
    row = weighted(weights_row, states_y)
    decays_z, states_z = unpack(sent_to_all(pack(decay_row, row), "sp_0"))
    weights_y, decay_y = weights_before(decays_y, y)
    inside = weighted(weights_y, states_y)
    weights_z, decay_z = weights_before(decays_z, z)
    start = lax.dynamic_index_in_dim(initial_state, c, keepdims=False).T
    before = jnp.exp(decay_z)[None, :] * start + weighted(weights_z, states_z)
    into_chip = jnp.exp(decay_y)[None, :] * before + inside
    into_second = jnp.exp(decay_0)[None, :] * into_chip + state_0
    incoming = exchanged(jnp.stack([into_chip, into_second]).astype(bf16), "sp_2")

    rest = jnp.dot(
        jnp.concatenate([halo, own], axis=0), weights[:, 512:], preferred_element_type=f32
    ).astype(bf16)
    queries = rest[HALO:, :256].astype(f32)
    gate_out = rest[HALO:, 256:512].astype(f32)
    product = rest[:, 512:768].astype(f32) * rest[:, 768:].astype(f32)
    filtered = jnp.zeros_like(gate_out)
    for offset in range(TAPS):
        at = HALO - (TAPS - 1) + offset
        filtered = filtered + filter_taps[offset] * product[at : at + length]
    filter_out = (gate_out * filtered).astype(bf16)
    filter_part = jnp.dot(filter_out, w_out_filter, preferred_element_type=f32)

    heads = lambda a: a.reshape(length // SPAN, SPAN, 2, HEAD_DIM)
    running = running_sum(log_decay)
    at_start = jnp.concatenate([jnp.zeros((1, 256), f32), running[SPAN - 1 : length - 1 : SPAN]])
    at_end = running[SPAN - 1 :: SPAN]
    within = running.reshape(length // SPAN, SPAN, 256) - at_start[:, None]
    scaled_query = heads((queries.reshape(within.shape) * jnp.exp(within)).astype(bf16))
    scaled_key = heads((key_rate.reshape(within.shape) * jnp.exp(-within)).astype(bf16))
    remainder = heads(
        (
            key_rate.reshape(within.shape)
            * jnp.exp(at_end[:, None] - running.reshape(within.shape))
        ).astype(bf16)
    )
    values = heads(value_in.astype(bf16))
    causal = jnp.tril(jnp.ones((SPAN, SPAN), dtype=bool))
    scores = jnp.einsum("bthk,bshk->bhts", scaled_query, scaled_key, preferred_element_type=f32)
    scores = jnp.where(causal, scores, 0.0).astype(bf16)
    local = jnp.einsum("bhts,bshv->bthv", scores, values, preferred_element_type=f32)
    cross = jnp.einsum("thk,shk->hts", scaled_query[1], remainder[0], preferred_element_type=f32)
    cross = jnp.einsum("hts,shv->thv", cross.astype(bf16), values[0], preferred_element_type=f32)
    local = jnp.concatenate([local[0], local[1] + cross], axis=0)
    full_query = (queries * jnp.exp(running)).astype(bf16).reshape(length, 2, HEAD_DIM)
    raw = local + jnp.einsum("thk,hvk->thv", full_query, incoming, preferred_element_type=f32)
    rec_out = (
        (raw * lax.rsqrt(jnp.mean(raw * raw, axis=-1, keepdims=True) + epsilon) * head_gain)
        .astype(bf16)
        .reshape(length, -1)
    )
    partial = (filter_part + jnp.dot(rec_out, w_out_rec, preferred_element_type=f32)).astype(bf16)
    arrived = exchanged(partial.reshape(4, length // 4, -1), "tp")
    return arrived.astype(f32).sum(axis=0).astype(bf16)


def solution(mesh):
    torus = Mesh(mesh.devices.reshape(8, 8, 2, mesh.shape["tp"]), ("sp_0", "sp_1", "sp_2", "tp"))
    placed = (
        P(SP_TP, None),
        P(),
        P(SP, "tp"),
        P(SP, "tp"),
        P(SP, "tp"),
        P(None, "tp"),
        P(SP, "tp"),
        P(SP, "tp"),
        P(SP, "tp"),
        P("tp"),
        P(SP, "tp"),
        P(),
        P("tp", None, None),
        P("tp", None),
        P("tp", None),
    )
    return jax.shard_map(
        body, mesh=torus, in_specs=placed, out_specs=P(SP_TP, None), check_vma=False
    )
```

```python
import jax
import jax.numpy as jnp
import numpy as np
from jax import lax
from jax.sharding import Mesh
from jax.sharding import PartitionSpec as P

HEAD_DIM = 128
SPAN = 64
TAPS = 3
HALO = 16
SP = ("sp_0", "sp_1", "sp_2")
SP_TP = ("sp_0", "sp_1", "sp_2", "tp")

epsilon = 1e-06
f32 = jnp.float32
bf16 = jnp.bfloat16


def exchanged(blocks, axis):
    return lax.all_to_all(blocks, axis, split_axis=0, concat_axis=0, tiled=True)


def sent_to_all(x, axis):
    return exchanged(jnp.broadcast_to(x, (lax.axis_size(axis), *x.shape)), axis)


def swapped(x, axis):
    return lax.ppermute(x, axis, [(0, 1), (1, 0)])


def shifted(block, axis):
    size = lax.axis_size(axis)
    return lax.ppermute(block, axis, [(i, i + 1) for i in range(size - 1)])


def running_sum(x):
    causal = jnp.tril(jnp.ones((x.shape[0], x.shape[0]), f32))
    return jnp.dot(causal, x, precision=lax.Precision.HIGHEST)


def rates(forget_logit, forget_gap, fade):
    key_rate = forget_gap * jax.nn.sigmoid(-forget_logit.astype(f32))
    return key_rate, jnp.log1p(-key_rate) + fade


def silu(v):
    return jax.nn.silu(v.astype(f32))


def state_of(key_rate, log_decay, value_in):
    running = running_sum(log_decay)
    remainder = (key_rate * jnp.exp(running[-1:] - running)).astype(bf16)
    state = jnp.einsum("tv,tk->vk", value_in.astype(bf16), remainder, preferred_element_type=f32)
    return running[-1], state


def pack(decay, state):
    high = lax.reduce_precision(decay, 8, 7)
    rest = decay - high
    low = lax.reduce_precision(rest, 8, 7)
    rows = jnp.stack([high, low, rest - low]).astype(bf16)
    return jnp.concatenate([state.astype(bf16), rows, jnp.zeros((13, HEAD_DIM), bf16)], axis=0)


def unpack(packed):
    decays = packed[:, HEAD_DIM : HEAD_DIM + 3].astype(f32).sum(axis=1)
    return decays, packed[:, :HEAD_DIM]


def weights_before(decays, position):
    size = decays.shape[0]
    place = jnp.arange(size)
    earlier = place < position
    kept = jnp.where(earlier[:, None], decays, 0.0)
    after = (place[None, :] > place[:, None]).astype(f32)
    since = jnp.sum(after[:, :, None] * kept[None], axis=1)
    return jnp.where(earlier[:, None], jnp.exp(since), 0.0), kept.sum(axis=0)


def weighted(weights, states):
    return jnp.sum(weights[:, None, :] * states.astype(f32), axis=0)


def body(
    tokens,
    norm_gain,
    w_filter_b,
    w_filter_c,
    w_filter_v,
    filter_taps,
    w_query,
    retention_gate_matrix,
    w_input,
    forget_gap,
    additive_fade_log,
    head_gain,
    initial_state,
    w_out_filter,
    w_out_rec,
):
    z, y, c = (lax.axis_index(a) for a in SP)
    state_rows = jnp.concatenate([retention_gate_matrix, w_input], axis=1)
    state_along_y = sent_to_all(state_rows, "sp_1").reshape(-1, state_rows.shape[1])
    rest_rows = jnp.concatenate([w_query, w_filter_b, w_filter_c, w_filter_v], axis=1)
    state_along_y, rest_rows = lax.optimization_barrier((state_along_y, rest_rows))
    state_weights = lax.all_gather(state_along_y, ("sp_0", "sp_2"), axis=0, tiled=True)
    rest_along_y = sent_to_all(rest_rows, "sp_1").reshape(-1, rest_rows.shape[1])
    rest_weights = lax.all_gather(rest_along_y, ("sp_0", "sp_2"), axis=0, tiled=True)

    gathered = sent_to_all(tokens, "tp").reshape(-1, tokens.shape[1])
    widened = gathered.astype(f32)
    normed = (
        widened
        * lax.rsqrt(jnp.mean(widened * widened, axis=-1, keepdims=True) + epsilon)
        * norm_gain
    ).astype(bf16)
    length, width = normed.shape
    order = np.arange(256).reshape(8, 2, 16).transpose(1, 0, 2).reshape(-1)
    swap = np.zeros((256, 256), np.float32)
    swap[order, np.arange(256)] = 1.0
    own = jnp.einsum(
        "tzk,kl->tzl",
        normed.reshape(length, 8, 256),
        jnp.asarray(swap, bf16),
        preferred_element_type=f32,
    ).astype(bf16).reshape(length, width)
    partner = swapped(own, "sp_2")
    halo = shifted(own[length - HALO :], SP)

    fade = additive_fade_log
    head = lambda a, k: lax.dynamic_slice_in_dim(a, k * HEAD_DIM, HEAD_DIM, axis=1)
    partner_fade = swapped(head(fade, 1 - c), "sp_2")

    partner, halo, partner_fade = lax.optimization_barrier((partner, halo, partner_fade))

    chip = jnp.concatenate([own, partner], axis=0)
    chip_gates = jnp.dot(chip, state_weights, preferred_element_type=f32).astype(bf16)
    forget_logit, input_value = chip_gates[:, :256], chip_gates[:, 256:]
    key_rate, log_decay = rates(forget_logit[:length], forget_gap, fade)
    value_in = silu(input_value[:length])
    gap_c = lax.dynamic_slice_in_dim(forget_gap, c * HEAD_DIM, HEAD_DIM)
    partner_rate, partner_decay = rates(head(forget_logit[length:], c), gap_c, partner_fade)
    partner_value = silu(head(input_value[length:], c))
    decay_own, state_own = state_of(head(key_rate, c), head(log_decay, c), head(value_in, c))
    decay_partner, state_partner = state_of(partner_rate, partner_decay, partner_value)
    first = c == 0
    decay_0, decay_1 = (
        jnp.where(first, decay_own, decay_partner),
        jnp.where(first, decay_partner, decay_own),
    )
    state_0, state_1 = (
        jnp.where(first, state_own, state_partner),
        jnp.where(first, state_partner, state_own),
    )
    state_chip = jnp.exp(decay_1)[None, :] * state_0 + state_1

    decays_y, states_y = unpack(sent_to_all(pack(decay_0 + decay_1, state_chip), "sp_1"))
    weights_row, decay_row = weights_before(decays_y, 8)
    row = weighted(weights_row, states_y)
    decays_z, states_z = unpack(sent_to_all(pack(decay_row, row), "sp_0"))
    weights_y, decay_y = weights_before(decays_y, y)
    inside = weighted(weights_y, states_y)
    weights_z, decay_z = weights_before(decays_z, z)
    start = lax.dynamic_index_in_dim(initial_state, c, keepdims=False).T
    before = jnp.exp(decay_z)[None, :] * start + weighted(weights_z, states_z)
    into_chip = jnp.exp(decay_y)[None, :] * before + inside
    into_second = jnp.exp(decay_0)[None, :] * into_chip + state_0
    incoming = exchanged(jnp.stack([into_chip, into_second]).astype(bf16), "sp_2")

    rest = jnp.dot(
        jnp.concatenate([halo, own], axis=0), rest_weights, preferred_element_type=f32
    ).astype(bf16)
    queries = rest[HALO:, :256].astype(f32)
    gate_out = rest[HALO:, 256:512].astype(f32)
    product = rest[:, 512:768].astype(f32) * rest[:, 768:].astype(f32)
    filtered = jnp.zeros_like(gate_out)
    for offset in range(TAPS):
        at = HALO - (TAPS - 1) + offset
        filtered = filtered + filter_taps[offset] * product[at : at + length]
    filter_out = (gate_out * filtered).astype(bf16)
    filter_part = jnp.dot(filter_out, w_out_filter, preferred_element_type=f32)

    heads = lambda a: a.reshape(length // SPAN, SPAN, 2, HEAD_DIM)
    running = running_sum(log_decay)
    at_start = jnp.concatenate([jnp.zeros((1, 256), f32), running[SPAN - 1 : length - 1 : SPAN]])
    at_end = running[SPAN - 1 :: SPAN]
    within = running.reshape(length // SPAN, SPAN, 256) - at_start[:, None]
    scaled_query = heads((queries.reshape(within.shape) * jnp.exp(within)).astype(bf16))
    scaled_key = heads((key_rate.reshape(within.shape) * jnp.exp(-within)).astype(bf16))
    remainder = heads(
        (
            key_rate.reshape(within.shape)
            * jnp.exp(at_end[:, None] - running.reshape(within.shape))
        ).astype(bf16)
    )
    values = heads(value_in.astype(bf16))
    causal = jnp.tril(jnp.ones((SPAN, SPAN), dtype=bool))
    scores = jnp.einsum("bthk,bshk->bhts", scaled_query, scaled_key, preferred_element_type=f32)
    scores = jnp.where(causal, scores, 0.0).astype(bf16)
    local = jnp.einsum("bhts,bshv->bthv", scores, values, preferred_element_type=f32)
    cross = jnp.einsum("thk,shk->hts", scaled_query[1], remainder[0], preferred_element_type=f32)
    cross = jnp.einsum("hts,shv->thv", cross.astype(bf16), values[0], preferred_element_type=f32)
    local = jnp.concatenate([local[0], local[1] + cross], axis=0)
    full_query = (queries * jnp.exp(running)).astype(bf16).reshape(length, 2, HEAD_DIM)
    raw = local + jnp.einsum("thk,hvk->thv", full_query, incoming, preferred_element_type=f32)
    rec_out = (
        (raw * lax.rsqrt(jnp.mean(raw * raw, axis=-1, keepdims=True) + epsilon) * head_gain)
        .astype(bf16)
        .reshape(length, -1)
    )
    partial = (filter_part + jnp.dot(rec_out, w_out_rec, preferred_element_type=f32)).astype(bf16)
    arrived = exchanged(partial.reshape(4, length // 4, -1), "tp")
    return arrived.astype(f32).sum(axis=0).astype(bf16)


def solution(mesh):
    torus = Mesh(mesh.devices.reshape(8, 8, 2, mesh.shape["tp"]), ("sp_0", "sp_1", "sp_2", "tp"))
    placed = (
        P(SP_TP, None),
        P(),
        P(SP, "tp"),
        P(SP, "tp"),
        P(SP, "tp"),
        P(None, "tp"),
        P(SP, "tp"),
        P(SP, "tp"),
        P(SP, "tp"),
        P("tp"),
        P(SP, "tp"),
        P(),
        P("tp", None, None),
        P("tp", None),
        P("tp", None),
    )
    return jax.shard_map(
        body, mesh=torus, in_specs=placed, out_specs=P(SP_TP, None), check_vma=False
    )
```

```python
import jax
import jax.numpy as jnp
import numpy as np
from jax import lax
from jax.experimental import pallas as pl
from jax.experimental.pallas import tpu as pltpu
from jax.sharding import Mesh
from jax.sharding import PartitionSpec as P

HEAD_DIM = 128
SPAN = 64
TAPS = 3
HALO = 16
SP = ("sp_0", "sp_1", "sp_2")
SP_TP = ("sp_0", "sp_1", "sp_2", "tp")

epsilon = 1e-06
f32 = jnp.float32
bf16 = jnp.bfloat16


def exchanged(blocks, axis):
    return lax.all_to_all(blocks, axis, split_axis=0, concat_axis=0, tiled=True)


def sent_to_all(x, axis):
    return exchanged(jnp.broadcast_to(x, (lax.axis_size(axis), *x.shape)), axis)


def swapped(x, axis):
    return lax.ppermute(x, axis, [(0, 1), (1, 0)])


def shifted(block, axis):
    size = lax.axis_size(axis)
    return lax.ppermute(block, axis, [(i, i + 1) for i in range(size - 1)])


HIGHEST = lax.Precision.HIGHEST
ANY = pl.BlockSpec(memory_space=pl.ANY)
VMEM = pl.BlockSpec(memory_space=pltpu.VMEM)
SMEM = pl.BlockSpec(memory_space=pltpu.SMEM)
PIECES = 4
RATE, RUNNING, VALUE, STATE_0, INITIAL, DECAY_0, CARRIED = 0, 2, 4, 6, 7, 8, 9


def contracted(a, b, over):
    return lax.dot_general(a, b, ((over[0:1], over[1:2]), ((), ())), preferred_element_type=f32)


def running_sum(x):
    size = x.shape[0]
    row = lax.broadcasted_iota(jnp.int32, (size, size), 0)
    column = lax.broadcasted_iota(jnp.int32, (size, size), 1)
    causal = jnp.where(column <= row, 1.0, 0.0).astype(f32)
    return jnp.dot(causal, x, precision=HIGHEST, preferred_element_type=f32)


def sigmoid(v):
    return 1.0 / (1.0 + jnp.exp(-v))


def packed_rows(decay, state):
    high = decay.astype(bf16).astype(f32)
    rest = decay - high
    low = rest.astype(bf16).astype(f32)
    place = lax.broadcasted_iota(jnp.int32, (16, HEAD_DIM), 0)
    tail = jnp.where(place == 0, high, jnp.where(place == 1, low, rest - low))
    tail = jnp.where(place < 3, tail, 0.0)
    return jnp.concatenate([state, tail], axis=0).astype(bf16)


def state_kernel(
    core, own, partner, weights, gap, fade, partner_fade, initial,
    packed, carried,
    held, fade_held, initial_held, sems, small_sems,
):
    length = own.shape[0]
    piece = weights.shape[0] // PIECES
    copies = [
        pltpu.make_async_copy(weights.at[pl.ds(k * piece, piece)], held.at[k], sems.at[k])
        for k in range(PIECES)
    ]
    small_copies = [
        pltpu.make_async_copy(partner_fade, fade_held, small_sems.at[0]),
        pltpu.make_async_copy(initial.at[core[0]], initial_held, small_sems.at[1]),
    ]
    for copy in copies + small_copies:
        copy.start()
    rows = jnp.concatenate([own[...], partner[...]], axis=0)
    total = jnp.zeros((2 * length, weights.shape[1]), f32)
    for k in range(PIECES):
        copies[k].wait()
        total = total + jnp.dot(
            rows[:, k * piece : (k + 1) * piece], held[k], preferred_element_type=f32
        )
    for copy in small_copies:
        copy.wait()
    logits = total.astype(bf16).astype(f32)
    first = core[0] == 0

    def head(a):
        return jnp.where(first, a[:, :HEAD_DIM], a[:, HEAD_DIM:])

    wide = 2 * HEAD_DIM
    rate = gap[...] * sigmoid(-logits[:length, :wide])
    fall = jnp.log1p(-rate) + fade[...]
    value = logits[:length, wide:] * sigmoid(logits[:length, wide:])
    partner_rate = head(gap[...]) * sigmoid(-head(logits[length:, :wide]))
    partner_fall = jnp.log1p(-partner_rate) + fade_held[...]
    partner_value = head(logits[length:, wide:])
    partner_value = partner_value * sigmoid(partner_value)
    summed = running_sum(jnp.concatenate([fall, partner_fall], axis=1))
    running = summed[:, :wide]
    for h in range(2):
        cut = slice(h * HEAD_DIM, (h + 1) * HEAD_DIM)
        carried[RATE + h] = rate[:, cut]
        carried[RUNNING + h] = running[:, cut]
        carried[VALUE + h] = value[:, cut]
    carried[INITIAL] = initial_held[...].T

    def state_of(key, run, val):
        remainder = (key * jnp.exp(run[length - 1 :] - run)).astype(bf16)
        return run[length - 1 :], contracted(val.T.astype(bf16), remainder, (1, 0))

    own_decay, own_state = state_of(head(rate), head(running), head(value))
    next_decay, next_state = state_of(partner_rate, summed[:, wide:], partner_value)
    d0 = jnp.where(first, own_decay, next_decay)
    d1 = jnp.where(first, next_decay, own_decay)
    s0 = jnp.where(first, own_state, next_state)
    s1 = jnp.where(first, next_state, own_state)
    carried[DECAY_0, 0:1] = d0
    carried[STATE_0] = s0
    out = packed_rows(d0 + d1, jnp.exp(d1) * s0 + s1)
    for k in range(packed.shape[0]):
        packed[k] = out


def decay_at(arrived, k):
    tail = arrived[k, HEAD_DIM : HEAD_DIM + 16].astype(f32)
    place = lax.broadcasted_iota(jnp.int32, tail.shape, 0)
    return jnp.sum(jnp.where(place < 3, tail, 0.0), axis=0, keepdims=True)


def before_place(arrived, place):
    decay = jnp.zeros((1, HEAD_DIM), f32)
    state = jnp.zeros((HEAD_DIM, HEAD_DIM), f32)
    for k in reversed(range(arrived.shape[0])):
        weight = jnp.where(k < place, jnp.exp(decay), 0.0)
        state = state + weight * arrived[k, :HEAD_DIM].astype(f32)
        decay = decay + jnp.where(k < place, decay_at(arrived, k), 0.0)
    return decay, state


def row_kernel(place, arrived, carried, packed, decays, states):
    decay, state = before_place(arrived, arrived.shape[0])
    out = packed_rows(decay, state)
    for k in range(packed.shape[0]):
        packed[k] = out
    decay, state = before_place(arrived, place[0])
    decay_0 = carried[DECAY_0, 0:1]
    decays[0:1] = decay
    decays[1:2] = decay + decay_0
    states[0] = state
    states[1] = jnp.exp(decay_0) * state + carried[STATE_0]


def enter_kernel(place, arrived, carried, decays, states, incoming):
    decay, state = before_place(arrived, place[0])
    before = jnp.exp(decay) * carried[INITIAL] + state
    for k in range(2):
        incoming[k] = (jnp.exp(decays[k : k + 1]) * before + states[k]).astype(bf16)


def final_kernel(
    halo, own, weights, carried, taps, incoming, head_gain, w_filter, w_rec,
    partial,
    held, rows, out_filter, out_rec, sems, row_sems, out_sems,
):
    length = own.shape[0]
    piece = weights.shape[0] // PIECES
    row_copies = [
        pltpu.make_async_copy(halo, rows.at[pl.ds(0, HALO)], row_sems.at[0]),
        pltpu.make_async_copy(own, rows.at[pl.ds(HALO, length)], row_sems.at[1]),
    ]
    out_copies = [
        pltpu.make_async_copy(w_filter, out_filter, out_sems.at[0]),
        pltpu.make_async_copy(w_rec, out_rec, out_sems.at[1]),
    ]
    for copy in row_copies:
        copy.start()
    copies = [
        pltpu.make_async_copy(weights.at[pl.ds(k * piece, piece)], held.at[k], sems.at[k])
        for k in range(PIECES)
    ]
    for copy in copies + out_copies:
        copy.start()
    for copy in row_copies:
        copy.wait()
    total = jnp.zeros((HALO + length, weights.shape[1]), f32)
    for k in range(PIECES):
        copies[k].wait()
        total = total + jnp.dot(
            rows[:, k * piece : (k + 1) * piece], held[k], preferred_element_type=f32
        )
    wide = 2 * HEAD_DIM
    rest = total.astype(bf16).astype(f32)
    product = rest[:, 2 * wide : 3 * wide] * rest[:, 3 * wide :]
    filtered = taps[TAPS - 1 : TAPS] * product
    for back in range(1, TAPS):
        at = TAPS - 1 - back
        filtered = filtered + taps[at : at + 1] * pltpu.roll(product, back, 0)
    filter_out = (rest[:, wide : 2 * wide] * filtered)[HALO:].astype(bf16)
    queries = rest[HALO:, :wide]
    mean = 1.0 / HEAD_DIM
    row = lax.broadcasted_iota(jnp.int32, (SPAN, SPAN), 0)
    column = lax.broadcasted_iota(jnp.int32, (SPAN, SPAN), 1)
    parts = []
    for h in range(2):
        cut = slice(h * HEAD_DIM, (h + 1) * HEAD_DIM)
        run = carried[RUNNING + h]
        rate = carried[RATE + h]
        value = carried[VALUE + h].astype(bf16)
        full = (queries[:, cut] * jnp.exp(run)).astype(bf16)
        blocks = []
        edge = jnp.zeros((1, HEAD_DIM), f32)
        earlier = None
        for b in range(length // SPAN):
            at = slice(b * SPAN, (b + 1) * SPAN)
            inside = run[at] - edge
            last = run[(b + 1) * SPAN - 1 : (b + 1) * SPAN]
            scaled_query = (queries[at, cut] * jnp.exp(inside)).astype(bf16)
            scaled_key = (rate[at] * jnp.exp(-inside)).astype(bf16)
            scores = contracted(scaled_query, scaled_key, (1, 1))
            scores = jnp.where(column <= row, scores, 0.0).astype(bf16)
            vals = value[at]
            local = jnp.dot(scores, vals, preferred_element_type=f32)
            if earlier is not None:
                across = contracted(scaled_query, earlier[0], (1, 1)).astype(bf16)
                local = local + jnp.dot(across, earlier[1], preferred_element_type=f32)
            remainder = (rate[at] * jnp.exp(last - run[at])).astype(bf16)
            earlier = (remainder, vals)
            edge = last
            blocks.append(local)
        raw = jnp.concatenate(blocks, axis=0) + contracted(full, incoming[h], (1, 1))
        scale = lax.rsqrt(jnp.sum(raw * raw, axis=-1, keepdims=True) * mean + epsilon)
        parts.append((raw * scale * head_gain[...]).astype(bf16))
    rec_out = jnp.concatenate(parts, axis=1)
    for copy in out_copies:
        copy.wait()
    partial[...] = (
        jnp.dot(filter_out, out_filter[...], preferred_element_type=f32)
        + jnp.dot(rec_out, out_rec[...], preferred_element_type=f32)
    ).astype(bf16)


def made(shape, kind):
    return pltpu.VMEM(shape, kind)


def granted(mebibytes):
    return pltpu.CompilerParams(vmem_limit_bytes=mebibytes * 2**20)


def far(x):
    return pltpu.with_memory_space_constraint(x, pltpu.HBM)


def near(x):
    return pltpu.with_memory_space_constraint(x, pltpu.VMEM)


def body(
    tokens,
    norm_gain,
    w_filter_b,
    w_filter_c,
    w_filter_v,
    filter_taps,
    w_query,
    retention_gate_matrix,
    w_input,
    forget_gap,
    additive_fade_log,
    head_gain,
    initial_state,
    w_out_filter,
    w_out_rec,
):
    z, y, c = (lax.axis_index(a) for a in SP)
    state_rows = jnp.concatenate([retention_gate_matrix, w_input], axis=1)
    state_along_y = sent_to_all(state_rows, "sp_1").reshape(-1, state_rows.shape[1])
    rest_rows = jnp.concatenate([w_query, w_filter_b, w_filter_c, w_filter_v], axis=1)
    state_along_y, rest_rows = lax.optimization_barrier((state_along_y, rest_rows))
    state_weights = lax.all_gather(state_along_y, ("sp_0", "sp_2"), axis=0, tiled=True)
    rest_along_y = sent_to_all(rest_rows, "sp_1").reshape(-1, rest_rows.shape[1])
    rest_weights = lax.all_gather(rest_along_y, ("sp_0", "sp_2"), axis=0, tiled=True)

    gathered = sent_to_all(tokens, "tp").reshape(-1, tokens.shape[1])
    widened = gathered.astype(f32)
    normed = (
        widened
        * lax.rsqrt(jnp.mean(widened * widened, axis=-1, keepdims=True) + epsilon)
        * norm_gain
    ).astype(bf16)
    length, width = normed.shape
    order = np.arange(256).reshape(8, 2, 16).transpose(1, 0, 2).reshape(-1)
    swap = np.zeros((256, 256), np.float32)
    swap[order, np.arange(256)] = 1.0
    own = jnp.einsum(
        "tzk,kl->tzl",
        normed.reshape(length, 8, 256),
        jnp.asarray(swap, bf16),
        preferred_element_type=f32,
    ).astype(bf16).reshape(length, width)
    partner = swapped(own, "sp_2")
    halo = shifted(own[length - HALO :], SP)

    fade = additive_fade_log
    head = lambda a, k: lax.dynamic_slice_in_dim(a, k * HEAD_DIM, HEAD_DIM, axis=1)
    partner_fade = swapped(head(fade, 1 - c), "sp_2")

    partner, halo, partner_fade = lax.optimization_barrier((partner, halo, partner_fade))

    core = jnp.stack([c])
    dma = pltpu.SemaphoreType.DMA
    square = (HEAD_DIM, HEAD_DIM)
    packed_shape = jax.ShapeDtypeStruct((8, HEAD_DIM + 16, HEAD_DIM), bf16)
    packed, carried = pl.pallas_call(
        state_kernel,
        in_specs=[SMEM, VMEM, VMEM, ANY, VMEM, VMEM, ANY, ANY],
        out_specs=[VMEM] * 2,
        out_shape=[packed_shape, made((CARRIED, *square), f32)],
        scratch_shapes=[
            pltpu.VMEM((PIECES, width // PIECES, 512), bf16),
            pltpu.VMEM(square, f32),
            pltpu.VMEM(square, f32),
            dma((PIECES,)),
            dma((2,)),
        ],
        name="chip_state",
        compiler_params=granted(12),
    )(
        core,
        near(own),
        near(partner),
        far(state_weights),
        near(forget_gap[None]),
        near(fade),
        far(partner_fade),
        far(initial_state),
    )

    packed, decays, states = pl.pallas_call(
        row_kernel,
        in_specs=[SMEM] + [VMEM] * 2,
        out_specs=[VMEM] * 3,
        out_shape=[packed_shape, made((8, HEAD_DIM), f32), made((2, *square), f32)],
        name="along_row",
        compiler_params=granted(4),
    )(jnp.stack([y]), near(exchanged(packed, "sp_1")), carried)
    incoming = pl.pallas_call(
        enter_kernel,
        in_specs=[SMEM] + [VMEM] * 4,
        out_specs=VMEM,
        out_shape=made((2, *square), bf16),
        name="enter_chip",
        compiler_params=granted(4),
    )(jnp.stack([z]), near(exchanged(packed, "sp_0")), carried, decays, states)
    incoming = exchanged(incoming, "sp_2")

    partial = pl.pallas_call(
        final_kernel,
        in_specs=[ANY, ANY, ANY] + [VMEM] * 4 + [ANY, ANY],
        out_specs=VMEM,
        out_shape=made((length, width), bf16),
        scratch_shapes=[
            pltpu.VMEM((PIECES, width // PIECES, 1024), bf16),
            pltpu.VMEM((HALO + length, width), bf16),
            pltpu.VMEM((256, width), bf16),
            pltpu.VMEM((256, width), bf16),
            dma((PIECES,)),
            dma((2,)),
            dma((2,)),
        ],
        name="outputs",
        compiler_params=granted(20),
    )(
        far(halo),
        far(own),
        far(rest_weights),
        carried,
        near(filter_taps),
        near(incoming),
        near(head_gain[None]),
        far(w_out_filter),
        far(w_out_rec),
    )
    arrived = exchanged(partial.reshape(4, length // 4, -1), "tp")
    return arrived.astype(f32).sum(axis=0).astype(bf16)


def solution(mesh):
    torus = Mesh(mesh.devices.reshape(8, 8, 2, mesh.shape["tp"]), ("sp_0", "sp_1", "sp_2", "tp"))
    placed = (
        P(SP_TP, None),
        P(),
        P(SP, "tp"),
        P(SP, "tp"),
        P(SP, "tp"),
        P(None, "tp"),
        P(SP, "tp"),
        P(SP, "tp"),
        P(SP, "tp"),
        P("tp"),
        P(SP, "tp"),
        P(),
        P("tp", None, None),
        P("tp", None),
        P("tp", None),
    )
    return jax.shard_map(
        body, mesh=torus, in_specs=placed, out_specs=P(SP_TP, None), check_vma=False
    )
```

```python
import jax
import jax.numpy as jnp
import numpy as np
from jax import lax
from jax.experimental import pallas as pl
from jax.experimental.pallas import tpu as pltpu
from jax.sharding import Mesh
from jax.sharding import PartitionSpec as P

HEAD_DIM = 128
SPAN = 64
TAPS = 3
HALO = 16
SP = ("sp_0", "sp_1", "sp_2")
SP_TP = ("sp_0", "sp_1", "sp_2", "tp")

epsilon = 1e-06
f32 = jnp.float32
bf16 = jnp.bfloat16


def exchanged(blocks, axis):
    return lax.all_to_all(blocks, axis, split_axis=0, concat_axis=0, tiled=True)


def sent_to_all(x, axis):
    return exchanged(jnp.broadcast_to(x, (lax.axis_size(axis), *x.shape)), axis)


def swapped(x, axis):
    return lax.ppermute(x, axis, [(0, 1), (1, 0)])


def shifted(block, axis):
    size = lax.axis_size(axis)
    return lax.ppermute(block, axis, [(i, i + 1) for i in range(size - 1)])


HIGHEST = lax.Precision.HIGHEST
ANY = pl.BlockSpec(memory_space=pl.ANY)
VMEM = pl.BlockSpec(memory_space=pltpu.VMEM)
SMEM = pl.BlockSpec(memory_space=pltpu.SMEM)
PIECES = 4
RATE, RUNNING, VALUE, STATE_0, INITIAL, DECAY_0, CARRIED = 0, 2, 4, 6, 7, 8, 9


def contracted(a, b, over):
    return lax.dot_general(a, b, ((over[0:1], over[1:2]), ((), ())), preferred_element_type=f32)


def running_sum(x):
    size = x.shape[0]
    row = lax.broadcasted_iota(jnp.int32, (size, size), 0)
    column = lax.broadcasted_iota(jnp.int32, (size, size), 1)
    causal = jnp.where(column <= row, 1.0, 0.0).astype(f32)
    return jnp.dot(causal, x, precision=HIGHEST, preferred_element_type=f32)


def sigmoid(v):
    return 1.0 / (1.0 + jnp.exp(-v))


def packed_rows(decay, state):
    high = decay.astype(bf16).astype(f32)
    rest = decay - high
    low = rest.astype(bf16).astype(f32)
    place = lax.broadcasted_iota(jnp.int32, (16, HEAD_DIM), 0)
    tail = jnp.where(place == 0, high, jnp.where(place == 1, low, rest - low))
    tail = jnp.where(place < 3, tail, 0.0)
    return jnp.concatenate([state, tail], axis=0).astype(bf16)


def state_kernel(
    places, own, partner, weights, gap, fade, partner_fade, initial,
    packed, carried,
    held, fade_held, initial_held, sems, small_sems,
):
    length = own.shape[0]
    piece = weights.shape[0] // PIECES
    copies = [
        pltpu.make_async_copy(weights.at[pl.ds(k * piece, piece)], held.at[k], sems.at[k])
        for k in range(PIECES)
    ]
    small_copies = [
        pltpu.make_async_copy(partner_fade, fade_held, small_sems.at[0]),
        pltpu.make_async_copy(initial.at[places[2]], initial_held, small_sems.at[1]),
    ]
    for copy in copies + small_copies:
        copy.start()
    rows = jnp.concatenate([own[...], partner[...]], axis=0)
    total = jnp.zeros((2 * length, weights.shape[1]), f32)
    for k in range(PIECES):
        copies[k].wait()
        total = total + jnp.dot(
            rows[:, k * piece : (k + 1) * piece], held[k], preferred_element_type=f32
        )
    for copy in small_copies:
        copy.wait()
    logits = total.astype(bf16).astype(f32)
    first = places[2] == 0

    def head(a):
        return jnp.where(first, a[:, :HEAD_DIM], a[:, HEAD_DIM:])

    wide = 2 * HEAD_DIM
    rate = gap[...] * sigmoid(-logits[:length, :wide])
    fall = jnp.log1p(-rate) + fade[...]
    value = logits[:length, wide:] * sigmoid(logits[:length, wide:])
    partner_rate = head(gap[...]) * sigmoid(-head(logits[length:, :wide]))
    partner_fall = jnp.log1p(-partner_rate) + fade_held[...]
    partner_value = head(logits[length:, wide:])
    partner_value = partner_value * sigmoid(partner_value)
    summed = running_sum(jnp.concatenate([fall, partner_fall], axis=1))
    running = summed[:, :wide]
    for h in range(2):
        cut = slice(h * HEAD_DIM, (h + 1) * HEAD_DIM)
        carried[RATE + h] = rate[:, cut]
        carried[RUNNING + h] = running[:, cut]
        carried[VALUE + h] = value[:, cut]
    carried[INITIAL] = initial_held[...].T

    def state_of(key, run, val):
        remainder = (key * jnp.exp(run[length - 1 :] - run)).astype(bf16)
        return run[length - 1 :], contracted(val.T.astype(bf16), remainder, (1, 0))

    own_decay, own_state = state_of(head(rate), head(running), head(value))
    next_decay, next_state = state_of(partner_rate, summed[:, wide:], partner_value)
    d0 = jnp.where(first, own_decay, next_decay)
    d1 = jnp.where(first, next_decay, own_decay)
    s0 = jnp.where(first, own_state, next_state)
    s1 = jnp.where(first, next_state, own_state)
    carried[DECAY_0, 0:1] = d0
    carried[STATE_0] = s0
    out = packed_rows(d0 + d1, jnp.exp(d1) * s0 + s1)
    for k in range(packed.shape[0]):
        packed[k] = out


def decay_at(arrived, k):
    tail = arrived[k, HEAD_DIM : HEAD_DIM + 16].astype(f32)
    place = lax.broadcasted_iota(jnp.int32, tail.shape, 0)
    return jnp.sum(jnp.where(place < 3, tail, 0.0), axis=0, keepdims=True)


def before_place(arrived, place):
    decay = jnp.zeros((1, HEAD_DIM), f32)
    state = jnp.zeros((HEAD_DIM, HEAD_DIM), f32)
    for k in reversed(range(arrived.shape[0])):
        weight = jnp.where(k < place, jnp.exp(decay), 0.0)
        state = state + weight * arrived[k, :HEAD_DIM].astype(f32)
        decay = decay + jnp.where(k < place, decay_at(arrived, k), 0.0)
    return decay, state


def row_kernel(places, arrived, carried, packed, decays, states):
    decay, state = before_place(arrived, arrived.shape[0])
    out = packed_rows(decay, state)
    for k in range(packed.shape[0]):
        packed[k] = out
    decay, state = before_place(arrived, places[1])
    decay_0 = carried[DECAY_0, 0:1]
    decays[0:1] = decay
    decays[1:2] = decay + decay_0
    states[0] = state
    states[1] = jnp.exp(decay_0) * state + carried[STATE_0]


def enter_kernel(places, arrived, carried, decays, states, incoming):
    decay, state = before_place(arrived, places[0])
    before = jnp.exp(decay) * carried[INITIAL] + state
    for k in range(2):
        incoming[k] = (jnp.exp(decays[k : k + 1]) * before + states[k]).astype(bf16)


def final_kernel(
    halo, own, weights, carried, taps, incoming, head_gain, w_filter, w_rec,
    partial,
    held, rows, out_rec, sems, row_sems, out_sems,
):
    length = own.shape[0]
    piece = weights.shape[0] // PIECES
    row_copies = [
        pltpu.make_async_copy(halo, rows.at[pl.ds(0, HALO)], row_sems.at[0]),
        pltpu.make_async_copy(own, rows.at[pl.ds(HALO, length)], row_sems.at[1]),
    ]
    out_copies = [
        pltpu.make_async_copy(w_rec, out_rec, out_sems.at[0]),
    ]
    for copy in row_copies:
        copy.start()
    copies = [
        pltpu.make_async_copy(weights.at[pl.ds(k * piece, piece)], held.at[k], sems.at[k])
        for k in range(PIECES)
    ]
    for copy in copies + out_copies:
        copy.start()
    for copy in row_copies:
        copy.wait()
    total = jnp.zeros((HALO + length, weights.shape[1]), f32)
    for k in range(PIECES):
        copies[k].wait()
        total = total + jnp.dot(
            rows[:, k * piece : (k + 1) * piece], held[k], preferred_element_type=f32
        )
    wide = 2 * HEAD_DIM
    rest = total.astype(bf16).astype(f32)
    product = rest[:, 2 * wide : 3 * wide] * rest[:, 3 * wide :]
    filtered = taps[TAPS - 1 : TAPS] * product
    for back in range(1, TAPS):
        at = TAPS - 1 - back
        filtered = filtered + taps[at : at + 1] * pltpu.roll(product, back, 0)
    filter_out = (rest[:, wide : 2 * wide] * filtered)[HALO:].astype(bf16)
    queries = rest[HALO:, :wide]
    mean = 1.0 / HEAD_DIM
    row = lax.broadcasted_iota(jnp.int32, (SPAN, SPAN), 0)
    column = lax.broadcasted_iota(jnp.int32, (SPAN, SPAN), 1)
    parts = []
    for h in range(2):
        cut = slice(h * HEAD_DIM, (h + 1) * HEAD_DIM)
        run = carried[RUNNING + h]
        rate = carried[RATE + h]
        value = carried[VALUE + h].astype(bf16)
        full = (queries[:, cut] * jnp.exp(run)).astype(bf16)
        blocks = []
        edge = jnp.zeros((1, HEAD_DIM), f32)
        earlier = None
        for b in range(length // SPAN):
            at = slice(b * SPAN, (b + 1) * SPAN)
            inside = run[at] - edge
            last = run[(b + 1) * SPAN - 1 : (b + 1) * SPAN]
            scaled_query = (queries[at, cut] * jnp.exp(inside)).astype(bf16)
            scaled_key = (rate[at] * jnp.exp(-inside)).astype(bf16)
            scores = contracted(scaled_query, scaled_key, (1, 1))
            scores = jnp.where(column <= row, scores, 0.0).astype(bf16)
            vals = value[at]
            local = jnp.dot(scores, vals, preferred_element_type=f32)
            if earlier is not None:
                across = contracted(scaled_query, earlier[0], (1, 1)).astype(bf16)
                local = local + jnp.dot(across, earlier[1], preferred_element_type=f32)
            remainder = (rate[at] * jnp.exp(last - run[at])).astype(bf16)
            earlier = (remainder, vals)
            edge = last
            blocks.append(local)
        raw = jnp.concatenate(blocks, axis=0) + contracted(full, incoming[h], (1, 1))
        scale = lax.rsqrt(jnp.sum(raw * raw, axis=-1, keepdims=True) * mean + epsilon)
        parts.append((raw * scale * head_gain[...]).astype(bf16))
    rec_out = jnp.concatenate(parts, axis=1)
    for copy in out_copies:
        copy.wait()
    partial[...] = (
        jnp.dot(filter_out, w_filter[...], preferred_element_type=f32)
        + jnp.dot(rec_out, out_rec[...], preferred_element_type=f32)
    ).astype(bf16)


def made(shape, kind):
    return pltpu.VMEM(shape, kind)


def granted(mebibytes):
    return pltpu.CompilerParams(vmem_limit_bytes=mebibytes * 2**20)


def far(x):
    return pltpu.with_memory_space_constraint(x, pltpu.HBM)


def near(x):
    return pltpu.with_memory_space_constraint(x, pltpu.VMEM)


def body(
    tokens,
    norm_gain,
    w_filter_b,
    w_filter_c,
    w_filter_v,
    filter_taps,
    w_query,
    retention_gate_matrix,
    w_input,
    forget_gap,
    additive_fade_log,
    head_gain,
    initial_state,
    w_out_filter,
    w_out_rec,
):
    z, y, c = (lax.axis_index(a) for a in SP)
    state_rows = jnp.concatenate([retention_gate_matrix, w_input], axis=1)
    state_along_y = sent_to_all(state_rows, "sp_1").reshape(-1, state_rows.shape[1])
    rest_rows = jnp.concatenate([w_query, w_filter_b, w_filter_c, w_filter_v], axis=1)
    state_along_y, rest_rows = lax.optimization_barrier((state_along_y, rest_rows))
    state_weights = lax.all_gather(state_along_y, ("sp_0", "sp_2"), axis=0, tiled=True)
    rest_along_y = sent_to_all(rest_rows, "sp_1").reshape(-1, rest_rows.shape[1])
    rest_weights = lax.all_gather(rest_along_y, ("sp_0", "sp_2"), axis=0, tiled=True)

    gathered = sent_to_all(tokens, "tp").reshape(-1, tokens.shape[1])
    widened = gathered.astype(f32)
    normed = (
        widened
        * lax.rsqrt(jnp.mean(widened * widened, axis=-1, keepdims=True) + epsilon)
        * norm_gain
    ).astype(bf16)
    length, width = normed.shape
    order = np.arange(256).reshape(8, 2, 16).transpose(1, 0, 2).reshape(-1)
    swap = np.zeros((256, 256), np.float32)
    swap[order, np.arange(256)] = 1.0
    own = jnp.einsum(
        "tzk,kl->tzl",
        normed.reshape(length, 8, 256),
        jnp.asarray(swap, bf16),
        preferred_element_type=f32,
    ).astype(bf16).reshape(length, width)
    partner = swapped(own, "sp_2")
    halo = shifted(own[length - HALO :], SP)

    fade = additive_fade_log
    head = lambda a, k: lax.dynamic_slice_in_dim(a, k * HEAD_DIM, HEAD_DIM, axis=1)
    partner_fade = swapped(head(fade, 1 - c), "sp_2")

    places = jnp.stack([z, y, c])
    partner, halo, partner_fade, places = lax.optimization_barrier(
        (partner, halo, partner_fade, places)
    )

    dma = pltpu.SemaphoreType.DMA
    square = (HEAD_DIM, HEAD_DIM)
    packed_shape = jax.ShapeDtypeStruct((8, HEAD_DIM + 16, HEAD_DIM), bf16)
    packed, carried = pl.pallas_call(
        state_kernel,
        in_specs=[SMEM, VMEM, VMEM, ANY, VMEM, VMEM, ANY, ANY],
        out_specs=[VMEM] * 2,
        out_shape=[packed_shape, made((CARRIED, *square), f32)],
        scratch_shapes=[
            pltpu.VMEM((PIECES, width // PIECES, 512), bf16),
            pltpu.VMEM(square, f32),
            pltpu.VMEM(square, f32),
            dma((PIECES,)),
            dma((2,)),
        ],
        name="chip_state",
        compiler_params=granted(12),
    )(
        places,
        near(own),
        near(partner),
        far(state_weights),
        near(forget_gap[None]),
        near(fade),
        far(partner_fade),
        far(initial_state),
    )

    packed, decays, states = pl.pallas_call(
        row_kernel,
        in_specs=[SMEM] + [VMEM] * 2,
        out_specs=[VMEM] * 3,
        out_shape=[packed_shape, made((8, HEAD_DIM), f32), made((2, *square), f32)],
        name="along_row",
        compiler_params=granted(4),
    )(places, near(exchanged(packed, "sp_1")), carried)
    incoming = pl.pallas_call(
        enter_kernel,
        in_specs=[SMEM] + [VMEM] * 4,
        out_specs=VMEM,
        out_shape=made((2, *square), bf16),
        name="enter_chip",
        compiler_params=granted(4),
    )(places, near(exchanged(packed, "sp_0")), carried, decays, states)
    incoming = exchanged(incoming, "sp_2")

    partial = pl.pallas_call(
        final_kernel,
        in_specs=[ANY, ANY, ANY] + [VMEM] * 5 + [ANY],
        out_specs=VMEM,
        out_shape=made((length, width), bf16),
        scratch_shapes=[
            pltpu.VMEM((PIECES, width // PIECES, 1024), bf16),
            pltpu.VMEM((HALO + length, width), bf16),
            pltpu.VMEM((256, width), bf16),
            dma((PIECES,)),
            dma((2,)),
            dma((1,)),
        ],
        name="outputs",
        compiler_params=granted(20),
    )(
        far(halo),
        far(own),
        far(rest_weights),
        carried,
        near(filter_taps),
        near(incoming),
        near(head_gain[None]),
        near(w_out_filter),
        far(w_out_rec),
    )
    arrived = exchanged(partial.reshape(4, length // 4, -1), "tp")
    return arrived.astype(f32).sum(axis=0).astype(bf16)


def solution(mesh):
    torus = Mesh(mesh.devices.reshape(8, 8, 2, mesh.shape["tp"]), ("sp_0", "sp_1", "sp_2", "tp"))
    placed = (
        P(SP_TP, None),
        P(),
        P(SP, "tp"),
        P(SP, "tp"),
        P(SP, "tp"),
        P(None, "tp"),
        P(SP, "tp"),
        P(SP, "tp"),
        P(SP, "tp"),
        P("tp"),
        P(SP, "tp"),
        P(),
        P("tp", None, None),
        P("tp", None),
        P("tp", None),
    )
    return jax.shard_map(
        body, mesh=torus, in_specs=placed, out_specs=P(SP_TP, None), check_vma=False
    )
```

```python
import jax
import jax.numpy as jnp
import numpy as np
from jax import lax
from jax.experimental import pallas as pl
from jax.experimental.pallas import tpu as pltpu
from jax.sharding import Mesh
from jax.sharding import PartitionSpec as P

HEAD_DIM = 128
SPAN = 64
TAPS = 3
HALO = 16
SP = ("sp_0", "sp_1", "sp_2")
SP_TP = ("sp_0", "sp_1", "sp_2", "tp")

epsilon = 1e-06
f32 = jnp.float32
bf16 = jnp.bfloat16


def exchanged(blocks, axis):
    return lax.all_to_all(blocks, axis, split_axis=0, concat_axis=0, tiled=True)


def sent_to_all(x, axis):
    return exchanged(jnp.broadcast_to(x, (lax.axis_size(axis), *x.shape)), axis)


def swapped(x, axis):
    return lax.ppermute(x, axis, [(0, 1), (1, 0)])


def shifted(block, axis):
    size = lax.axis_size(axis)
    return lax.ppermute(block, axis, [(i, i + 1) for i in range(size - 1)])


HIGHEST = lax.Precision.HIGHEST
ANY = pl.BlockSpec(memory_space=pl.ANY)
VMEM = pl.BlockSpec(memory_space=pltpu.VMEM)
SMEM = pl.BlockSpec(memory_space=pltpu.SMEM)
PIECES = 2
RATE, RUNNING, VALUE, STATE_0, INITIAL, DECAY_0, CARRIED = 0, 2, 4, 6, 7, 8, 9


def contracted(a, b, over):
    return lax.dot_general(a, b, ((over[0:1], over[1:2]), ((), ())), preferred_element_type=f32)


def running_sum(x):
    size = x.shape[0]
    row = lax.broadcasted_iota(jnp.int32, (size, size), 0)
    column = lax.broadcasted_iota(jnp.int32, (size, size), 1)
    causal = jnp.where(column <= row, 1.0, 0.0).astype(f32)
    return jnp.dot(causal, x, precision=HIGHEST, preferred_element_type=f32)


def sigmoid(v):
    return 1.0 / (1.0 + jnp.exp(-v))


def packed_rows(decay, state):
    high = decay.astype(bf16).astype(f32)
    rest = decay - high
    low = rest.astype(bf16).astype(f32)
    place = lax.broadcasted_iota(jnp.int32, (16, HEAD_DIM), 0)
    tail = jnp.where(place == 0, high, jnp.where(place == 1, low, rest - low))
    tail = jnp.where(place < 3, tail, 0.0)
    return jnp.concatenate([state, tail], axis=0).astype(bf16)


def state_kernel(
    places, own, partner, weights, gap, fade, partner_fade, initial,
    packed, carried,
    held, fade_held, initial_held, sems, small_sems,
):
    length = own.shape[0]
    piece = weights.shape[0] // PIECES
    copies = [
        pltpu.make_async_copy(weights.at[pl.ds(k * piece, piece)], held.at[k], sems.at[k])
        for k in range(PIECES)
    ]
    small_copies = [
        pltpu.make_async_copy(partner_fade, fade_held, small_sems.at[0]),
        pltpu.make_async_copy(initial.at[places[2]], initial_held, small_sems.at[1]),
    ]
    for copy in copies + small_copies:
        copy.start()
    rows = jnp.concatenate([own[...], partner[...]], axis=0)
    total = jnp.zeros((2 * length, weights.shape[1]), f32)
    for k in range(PIECES):
        copies[k].wait()
        total = total + jnp.dot(
            rows[:, k * piece : (k + 1) * piece], held[k], preferred_element_type=f32
        )
    for copy in small_copies:
        copy.wait()
    logits = total.astype(bf16).astype(f32)
    first = places[2] == 0

    def head(a):
        return jnp.where(first, a[:, :HEAD_DIM], a[:, HEAD_DIM:])

    wide = 2 * HEAD_DIM
    rate = gap[...] * sigmoid(-logits[:length, :wide])
    fall = jnp.log1p(-rate) + fade[...]
    value = logits[:length, wide:] * sigmoid(logits[:length, wide:])
    partner_rate = head(gap[...]) * sigmoid(-head(logits[length:, :wide]))
    partner_fall = jnp.log1p(-partner_rate) + fade_held[...]
    partner_value = head(logits[length:, wide:])
    partner_value = partner_value * sigmoid(partner_value)
    summed = running_sum(jnp.concatenate([fall, partner_fall], axis=1))
    running = summed[:, :wide]
    for h in range(2):
        cut = slice(h * HEAD_DIM, (h + 1) * HEAD_DIM)
        carried[RATE + h] = rate[:, cut]
        carried[RUNNING + h] = running[:, cut]
        carried[VALUE + h] = value[:, cut]
    carried[INITIAL] = initial_held[...].T

    def state_of(key, run, val):
        remainder = (key * jnp.exp(run[length - 1 :] - run)).astype(bf16)
        return run[length - 1 :], contracted(val.T.astype(bf16), remainder, (1, 0))

    own_decay, own_state = state_of(head(rate), head(running), head(value))
    next_decay, next_state = state_of(partner_rate, summed[:, wide:], partner_value)
    d0 = jnp.where(first, own_decay, next_decay)
    d1 = jnp.where(first, next_decay, own_decay)
    s0 = jnp.where(first, own_state, next_state)
    s1 = jnp.where(first, next_state, own_state)
    carried[DECAY_0, 0:1] = d0
    carried[STATE_0] = s0
    out = packed_rows(d0 + d1, jnp.exp(d1) * s0 + s1)
    for k in range(packed.shape[0]):
        packed[k] = out


def decay_at(arrived, k):
    tail = arrived[k, HEAD_DIM : HEAD_DIM + 16].astype(f32)
    place = lax.broadcasted_iota(jnp.int32, tail.shape, 0)
    return jnp.sum(jnp.where(place < 3, tail, 0.0), axis=0, keepdims=True)


def before_place(arrived, place):
    decay = jnp.zeros((1, HEAD_DIM), f32)
    state = jnp.zeros((HEAD_DIM, HEAD_DIM), f32)
    for k in reversed(range(arrived.shape[0])):
        weight = jnp.where(k < place, jnp.exp(decay), 0.0)
        state = state + weight * arrived[k, :HEAD_DIM].astype(f32)
        decay = decay + jnp.where(k < place, decay_at(arrived, k), 0.0)
    return decay, state


def row_kernel(places, arrived, carried, packed, decays, states):
    decay, state = before_place(arrived, arrived.shape[0])
    out = packed_rows(decay, state)
    for k in range(packed.shape[0]):
        packed[k] = out
    decay, state = before_place(arrived, places[1])
    decay_0 = carried[DECAY_0, 0:1]
    decays[0:1] = decay
    decays[1:2] = decay + decay_0
    states[0] = state
    states[1] = jnp.exp(decay_0) * state + carried[STATE_0]


def enter_kernel(places, arrived, carried, decays, states, incoming):
    decay, state = before_place(arrived, places[0])
    before = jnp.exp(decay) * carried[INITIAL] + state
    for k in range(2):
        incoming[k] = (jnp.exp(decays[k : k + 1]) * before + states[k]).astype(bf16)


def final_kernel(
    halo, own, weights, carried, taps, incoming, head_gain, w_filter, w_rec,
    partial,
    held, rows, out_rec, sems, row_sems, out_sems,
):
    length = own.shape[0]
    piece = weights.shape[0] // PIECES
    row_copies = [
        pltpu.make_async_copy(halo, rows.at[pl.ds(0, HALO)], row_sems.at[0]),
        pltpu.make_async_copy(own, rows.at[pl.ds(HALO, length)], row_sems.at[1]),
    ]
    out_copies = [
        pltpu.make_async_copy(w_rec, out_rec, out_sems.at[0]),
    ]
    for copy in row_copies:
        copy.start()
    copies = [
        pltpu.make_async_copy(weights.at[pl.ds(k * piece, piece)], held.at[k], sems.at[k])
        for k in range(PIECES)
    ]
    for copy in copies + out_copies:
        copy.start()
    for copy in row_copies:
        copy.wait()
    total = jnp.zeros((HALO + length, weights.shape[1]), f32)
    for k in range(PIECES):
        copies[k].wait()
        total = total + jnp.dot(
            rows[:, k * piece : (k + 1) * piece], held[k], preferred_element_type=f32
        )
    wide = 2 * HEAD_DIM
    rest = total.astype(bf16).astype(f32)
    product = rest[:, 2 * wide : 3 * wide] * rest[:, 3 * wide :]
    filtered = taps[TAPS - 1 : TAPS] * product
    for back in range(1, TAPS):
        at = TAPS - 1 - back
        filtered = filtered + taps[at : at + 1] * pltpu.roll(product, back, 0)
    filter_out = (rest[:, wide : 2 * wide] * filtered)[HALO:].astype(bf16)
    queries = rest[HALO:, :wide]
    mean = 1.0 / HEAD_DIM
    row = lax.broadcasted_iota(jnp.int32, (SPAN, SPAN), 0)
    column = lax.broadcasted_iota(jnp.int32, (SPAN, SPAN), 1)
    parts = []
    for h in range(2):
        cut = slice(h * HEAD_DIM, (h + 1) * HEAD_DIM)
        run = carried[RUNNING + h]
        rate = carried[RATE + h]
        value = carried[VALUE + h].astype(bf16)
        full = (queries[:, cut] * jnp.exp(run)).astype(bf16)
        blocks = []
        edge = jnp.zeros((1, HEAD_DIM), f32)
        earlier = None
        for b in range(length // SPAN):
            at = slice(b * SPAN, (b + 1) * SPAN)
            inside = run[at] - edge
            last = run[(b + 1) * SPAN - 1 : (b + 1) * SPAN]
            scaled_query = (queries[at, cut] * jnp.exp(inside)).astype(bf16)
            scaled_key = (rate[at] * jnp.exp(-inside)).astype(bf16)
            scores = contracted(scaled_query, scaled_key, (1, 1))
            scores = jnp.where(column <= row, scores, 0.0).astype(bf16)
            vals = value[at]
            local = jnp.dot(scores, vals, preferred_element_type=f32)
            if earlier is not None:
                across = contracted(scaled_query, earlier[0], (1, 1)).astype(bf16)
                local = local + jnp.dot(across, earlier[1], preferred_element_type=f32)
            remainder = (rate[at] * jnp.exp(last - run[at])).astype(bf16)
            earlier = (remainder, vals)
            edge = last
            blocks.append(local)
        raw = jnp.concatenate(blocks, axis=0) + contracted(full, incoming[h], (1, 1))
        scale = lax.rsqrt(jnp.sum(raw * raw, axis=-1, keepdims=True) * mean + epsilon)
        parts.append((raw * scale * head_gain[...]).astype(bf16))
    rec_out = jnp.concatenate(parts, axis=1)
    for copy in out_copies:
        copy.wait()
    partial[...] = (
        jnp.dot(filter_out, w_filter[...], preferred_element_type=f32)
        + jnp.dot(rec_out, out_rec[...], preferred_element_type=f32)
    ).astype(bf16)


def made(shape, kind):
    return pltpu.VMEM(shape, kind)


def granted(mebibytes):
    return pltpu.CompilerParams(vmem_limit_bytes=mebibytes * 2**20)


def far(x):
    return pltpu.with_memory_space_constraint(x, pltpu.HBM)


def near(x):
    return pltpu.with_memory_space_constraint(x, pltpu.VMEM)


def body(
    tokens,
    norm_gain,
    w_filter_b,
    w_filter_c,
    w_filter_v,
    filter_taps,
    w_query,
    retention_gate_matrix,
    w_input,
    forget_gap,
    additive_fade_log,
    head_gain,
    initial_state,
    w_out_filter,
    w_out_rec,
):
    z, y, c = (lax.axis_index(a) for a in SP)
    state_rows = jnp.concatenate([retention_gate_matrix, w_input], axis=1)
    state_along_y = sent_to_all(state_rows, "sp_1").reshape(-1, state_rows.shape[1])
    rest_rows = jnp.concatenate([w_query, w_filter_b, w_filter_c, w_filter_v], axis=1)
    state_along_y, rest_rows = lax.optimization_barrier((state_along_y, rest_rows))
    state_weights = lax.all_gather(state_along_y, ("sp_0", "sp_2"), axis=0, tiled=True)
    rest_along_y = sent_to_all(rest_rows, "sp_1").reshape(-1, rest_rows.shape[1])
    rest_weights = lax.all_gather(rest_along_y, ("sp_0", "sp_2"), axis=0, tiled=True)

    gathered = sent_to_all(tokens, "tp").reshape(-1, tokens.shape[1])
    widened = gathered.astype(f32)
    normed = (
        widened
        * lax.rsqrt(jnp.mean(widened * widened, axis=-1, keepdims=True) + epsilon)
        * norm_gain
    ).astype(bf16)
    length, width = normed.shape
    order = np.arange(256).reshape(8, 2, 16).transpose(1, 0, 2).reshape(-1)
    swap = np.zeros((256, 256), np.float32)
    swap[order, np.arange(256)] = 1.0
    own = jnp.einsum(
        "tzk,kl->tzl",
        normed.reshape(length, 8, 256),
        jnp.asarray(swap, bf16),
        preferred_element_type=f32,
    ).astype(bf16).reshape(length, width)
    partner = swapped(own, "sp_2")
    halo = shifted(own[length - HALO :], SP)

    fade = additive_fade_log
    head = lambda a, k: lax.dynamic_slice_in_dim(a, k * HEAD_DIM, HEAD_DIM, axis=1)
    partner_fade = swapped(head(fade, 1 - c), "sp_2")

    places = jnp.stack([z, y, c])
    partner, halo, partner_fade, places = lax.optimization_barrier(
        (partner, halo, partner_fade, places)
    )

    dma = pltpu.SemaphoreType.DMA
    square = (HEAD_DIM, HEAD_DIM)
    packed_shape = jax.ShapeDtypeStruct((8, HEAD_DIM + 16, HEAD_DIM), bf16)
    packed, carried = pl.pallas_call(
        state_kernel,
        in_specs=[SMEM, VMEM, VMEM, ANY, VMEM, VMEM, ANY, ANY],
        out_specs=[VMEM] * 2,
        out_shape=[packed_shape, made((CARRIED, *square), f32)],
        scratch_shapes=[
            pltpu.VMEM((PIECES, width // PIECES, 512), bf16),
            pltpu.VMEM(square, f32),
            pltpu.VMEM(square, f32),
            dma((PIECES,)),
            dma((2,)),
        ],
        name="chip_state",
        compiler_params=granted(12),
    )(
        places,
        near(own),
        near(partner),
        far(state_weights),
        near(forget_gap[None]),
        near(fade),
        far(partner_fade),
        far(initial_state),
    )

    packed, decays, states = pl.pallas_call(
        row_kernel,
        in_specs=[SMEM] + [VMEM] * 2,
        out_specs=[VMEM] * 3,
        out_shape=[packed_shape, made((8, HEAD_DIM), f32), made((2, *square), f32)],
        name="along_row",
        compiler_params=granted(4),
    )(places, near(exchanged(packed, "sp_1")), carried)
    incoming = pl.pallas_call(
        enter_kernel,
        in_specs=[SMEM] + [VMEM] * 4,
        out_specs=VMEM,
        out_shape=made((2, *square), bf16),
        name="enter_chip",
        compiler_params=granted(4),
    )(places, near(exchanged(packed, "sp_0")), carried, decays, states)
    incoming = exchanged(incoming, "sp_2")

    partial = pl.pallas_call(
        final_kernel,
        in_specs=[ANY, ANY, ANY] + [VMEM] * 5 + [ANY],
        out_specs=VMEM,
        out_shape=made((length, width), bf16),
        scratch_shapes=[
            pltpu.VMEM((PIECES, width // PIECES, 1024), bf16),
            pltpu.VMEM((HALO + length, width), bf16),
            pltpu.VMEM((256, width), bf16),
            dma((PIECES,)),
            dma((2,)),
            dma((1,)),
        ],
        name="outputs",
        compiler_params=granted(20),
    )(
        far(halo),
        far(own),
        far(rest_weights),
        carried,
        near(filter_taps),
        near(incoming),
        near(head_gain[None]),
        near(w_out_filter),
        far(w_out_rec),
    )
    arrived = exchanged(partial.reshape(4, length // 4, -1), "tp")
    return arrived.astype(f32).sum(axis=0).astype(bf16)


def solution(mesh):
    torus = Mesh(mesh.devices.reshape(8, 8, 2, mesh.shape["tp"]), ("sp_0", "sp_1", "sp_2", "tp"))
    placed = (
        P(SP_TP, None),
        P(),
        P(SP, "tp"),
        P(SP, "tp"),
        P(SP, "tp"),
        P(None, "tp"),
        P(SP, "tp"),
        P(SP, "tp"),
        P(SP, "tp"),
        P("tp"),
        P(SP, "tp"),
        P(),
        P("tp", None, None),
        P("tp", None),
        P("tp", None),
    )
    return jax.shard_map(
        body, mesh=torus, in_specs=placed, out_specs=P(SP_TP, None), check_vma=False
    )
```

```python
import jax
import jax.numpy as jnp
import numpy as np
from jax import lax
from jax.experimental import pallas as pl
from jax.experimental.pallas import tpu as pltpu
from jax.sharding import Mesh
from jax.sharding import PartitionSpec as P

HEAD_DIM = 128
SPAN = 64
TAPS = 3
HALO = 16
SP = ("sp_0", "sp_1", "sp_2")
SP_TP = ("sp_0", "sp_1", "sp_2", "tp")

epsilon = 1e-06
f32 = jnp.float32
bf16 = jnp.bfloat16


def exchanged(blocks, axis):
    return lax.all_to_all(blocks, axis, split_axis=0, concat_axis=0, tiled=True)


def sent_to_all(x, axis):
    return exchanged(jnp.broadcast_to(x, (lax.axis_size(axis), *x.shape)), axis)


def swapped(x, axis):
    return lax.ppermute(x, axis, [(0, 1), (1, 0)])


def shifted(block, axis):
    size = lax.axis_size(axis)
    return lax.ppermute(block, axis, [(i, i + 1) for i in range(size - 1)])


HIGHEST = lax.Precision.HIGHEST
ANY = pl.BlockSpec(memory_space=pl.ANY)
VMEM = pl.BlockSpec(memory_space=pltpu.VMEM)
SMEM = pl.BlockSpec(memory_space=pltpu.SMEM)
PIECES = 4
RATE, RUNNING, VALUE, STATE_0, INITIAL, DECAY_0, CARRIED = 0, 2, 4, 6, 7, 8, 9


def contracted(a, b, over):
    return lax.dot_general(a, b, ((over[0:1], over[1:2]), ((), ())), preferred_element_type=f32)


def running_sum(x):
    size = x.shape[0]
    row = lax.broadcasted_iota(jnp.int32, (size, size), 0)
    column = lax.broadcasted_iota(jnp.int32, (size, size), 1)
    causal = jnp.where(column <= row, 1.0, 0.0).astype(f32)
    return jnp.dot(causal, x, precision=HIGHEST, preferred_element_type=f32)


def sigmoid(v):
    return 1.0 / (1.0 + jnp.exp(-v))


def packed_rows(decay, state):
    high = decay.astype(bf16).astype(f32)
    rest = decay - high
    low = rest.astype(bf16).astype(f32)
    place = lax.broadcasted_iota(jnp.int32, (16, HEAD_DIM), 0)
    tail = jnp.where(place == 0, high, jnp.where(place == 1, low, rest - low))
    tail = jnp.where(place < 3, tail, 0.0)
    return jnp.concatenate([state, tail], axis=0).astype(bf16)


def state_kernel(
    places, own, partner, weights, gap, fade, partner_fade, initial,
    packed, carried,
    held, fade_held, initial_held, sems, small_sems,
):
    length = own.shape[0]
    piece = weights.shape[0] // PIECES
    copies = [
        pltpu.make_async_copy(weights.at[pl.ds(k * piece, piece)], held.at[k], sems.at[k])
        for k in range(PIECES)
    ]
    small_copies = [
        pltpu.make_async_copy(partner_fade, fade_held, small_sems.at[0]),
        pltpu.make_async_copy(initial.at[places[2]], initial_held, small_sems.at[1]),
    ]
    for copy in copies + small_copies:
        copy.start()
    rows = jnp.concatenate([own[...], partner[...]], axis=0)
    total = jnp.zeros((2 * length, weights.shape[1]), f32)
    for k in range(PIECES):
        copies[k].wait()
        total = total + jnp.dot(
            rows[:, k * piece : (k + 1) * piece], held[k], preferred_element_type=f32
        )
    for copy in small_copies:
        copy.wait()
    logits = total.astype(bf16).astype(f32)
    first = places[2] == 0

    def head(a):
        return jnp.where(first, a[:, :HEAD_DIM], a[:, HEAD_DIM:])

    wide = 2 * HEAD_DIM
    rate = gap[...] * sigmoid(-logits[:length, :wide])
    fall = jnp.log1p(-rate) + fade[...]
    value = logits[:length, wide:] * sigmoid(logits[:length, wide:])
    partner_rate = head(gap[...]) * sigmoid(-head(logits[length:, :wide]))
    partner_fall = jnp.log1p(-partner_rate) + fade_held[...]
    partner_value = head(logits[length:, wide:])
    partner_value = partner_value * sigmoid(partner_value)
    summed = running_sum(jnp.concatenate([fall, partner_fall], axis=1))
    running = summed[:, :wide]
    for h in range(2):
        cut = slice(h * HEAD_DIM, (h + 1) * HEAD_DIM)
        carried[RATE + h] = rate[:, cut]
        carried[RUNNING + h] = running[:, cut]
        carried[VALUE + h] = value[:, cut]
    carried[INITIAL] = initial_held[...].T

    def state_of(key, run, val):
        remainder = (key * jnp.exp(run[length - 1 :] - run)).astype(bf16)
        return run[length - 1 :], contracted(val.T.astype(bf16), remainder, (1, 0))

    own_decay, own_state = state_of(head(rate), head(running), head(value))
    next_decay, next_state = state_of(partner_rate, summed[:, wide:], partner_value)
    d0 = jnp.where(first, own_decay, next_decay)
    d1 = jnp.where(first, next_decay, own_decay)
    s0 = jnp.where(first, own_state, next_state)
    s1 = jnp.where(first, next_state, own_state)
    carried[DECAY_0, 0:1] = d0
    carried[STATE_0] = s0
    out = packed_rows(d0 + d1, jnp.exp(d1) * s0 + s1)
    for k in range(packed.shape[0]):
        packed[k] = out


def decay_at(arrived, k):
    tail = arrived[k, HEAD_DIM : HEAD_DIM + 16].astype(f32)
    place = lax.broadcasted_iota(jnp.int32, tail.shape, 0)
    return jnp.sum(jnp.where(place < 3, tail, 0.0), axis=0, keepdims=True)


def before_place(arrived, place):
    decay = jnp.zeros((1, HEAD_DIM), f32)
    state = jnp.zeros((HEAD_DIM, HEAD_DIM), f32)
    for k in reversed(range(arrived.shape[0])):
        weight = jnp.where(k < place, jnp.exp(decay), 0.0)
        state = state + weight * arrived[k, :HEAD_DIM].astype(f32)
        decay = decay + jnp.where(k < place, decay_at(arrived, k), 0.0)
    return decay, state


def row_kernel(places, arrived, carried, packed, decays, states):
    decay, state = before_place(arrived, arrived.shape[0])
    out = packed_rows(decay, state)
    for k in range(packed.shape[0]):
        packed[k] = out
    decay, state = before_place(arrived, places[1])
    decay_0 = carried[DECAY_0, 0:1]
    decays[0:1] = decay
    decays[1:2] = decay + decay_0
    states[0] = state
    states[1] = jnp.exp(decay_0) * state + carried[STATE_0]


def enter_kernel(places, arrived, carried, decays, states, incoming):
    decay, state = before_place(arrived, places[0])
    before = jnp.exp(decay) * carried[INITIAL] + state
    for k in range(2):
        incoming[k] = (jnp.exp(decays[k : k + 1]) * before + states[k]).astype(bf16)


def final_kernel(
    halo, own, weights, carried, taps, incoming, head_gain, w_filter, w_rec,
    partial,
    held, rows, out_rec, sems, row_sems, out_sems,
):
    length = own.shape[0]
    piece = weights.shape[0] // PIECES
    row_copies = [
        pltpu.make_async_copy(halo, rows.at[pl.ds(0, HALO)], row_sems.at[0]),
        pltpu.make_async_copy(own, rows.at[pl.ds(HALO, length)], row_sems.at[1]),
    ]
    out_copies = [
        pltpu.make_async_copy(w_rec, out_rec, out_sems.at[0]),
    ]
    for copy in row_copies:
        copy.start()
    copies = [
        pltpu.make_async_copy(weights.at[pl.ds(k * piece, piece)], held.at[k], sems.at[k])
        for k in range(PIECES)
    ]
    for copy in copies + out_copies:
        copy.start()
    for copy in row_copies:
        copy.wait()
    total = jnp.zeros((HALO + length, weights.shape[1]), f32)
    for k in range(PIECES):
        copies[k].wait()
        total = total + jnp.dot(
            rows[:, k * piece : (k + 1) * piece], held[k], preferred_element_type=f32
        )
    wide = 2 * HEAD_DIM
    rest = total.astype(bf16).astype(f32)
    product = rest[:, 2 * wide : 3 * wide] * rest[:, 3 * wide :]
    filtered = taps[TAPS - 1 : TAPS] * product
    for back in range(1, TAPS):
        at = TAPS - 1 - back
        filtered = filtered + taps[at : at + 1] * pltpu.roll(product, back, 0)
    filter_out = (rest[:, wide : 2 * wide] * filtered)[HALO:].astype(bf16)
    queries = rest[HALO:, :wide]
    mean = 1.0 / HEAD_DIM
    row = lax.broadcasted_iota(jnp.int32, (SPAN, SPAN), 0)
    column = lax.broadcasted_iota(jnp.int32, (SPAN, SPAN), 1)
    parts = []
    for h in range(2):
        cut = slice(h * HEAD_DIM, (h + 1) * HEAD_DIM)
        run = carried[RUNNING + h]
        rate = carried[RATE + h]
        value = carried[VALUE + h].astype(bf16)
        full = (queries[:, cut] * jnp.exp(run)).astype(bf16)
        blocks = []
        edge = jnp.zeros((1, HEAD_DIM), f32)
        earlier = None
        for b in range(length // SPAN):
            at = slice(b * SPAN, (b + 1) * SPAN)
            inside = run[at] - edge
            last = run[(b + 1) * SPAN - 1 : (b + 1) * SPAN]
            scaled_query = (queries[at, cut] * jnp.exp(inside)).astype(bf16)
            scaled_key = (rate[at] * jnp.exp(-inside)).astype(bf16)
            scores = contracted(scaled_query, scaled_key, (1, 1))
            scores = jnp.where(column <= row, scores, 0.0).astype(bf16)
            vals = value[at]
            local = jnp.dot(scores, vals, preferred_element_type=f32)
            if earlier is not None:
                across = contracted(scaled_query, earlier[0], (1, 1)).astype(bf16)
                local = local + jnp.dot(across, earlier[1], preferred_element_type=f32)
            remainder = (rate[at] * jnp.exp(last - run[at])).astype(bf16)
            earlier = (remainder, vals)
            edge = last
            blocks.append(local)
        raw = jnp.concatenate(blocks, axis=0) + contracted(full, incoming[h], (1, 1))
        scale = lax.rsqrt(jnp.sum(raw * raw, axis=-1, keepdims=True) * mean + epsilon)
        parts.append((raw * scale * head_gain[...]).astype(bf16))
    rec_out = jnp.concatenate(parts, axis=1)
    for copy in out_copies:
        copy.wait()
    partial[...] = (
        jnp.dot(filter_out, w_filter[...], preferred_element_type=f32)
        + jnp.dot(rec_out, out_rec[...], preferred_element_type=f32)
    ).astype(bf16)


def made(shape, kind):
    return pltpu.VMEM(shape, kind)


def granted(mebibytes):
    return pltpu.CompilerParams(vmem_limit_bytes=mebibytes * 2**20)


def far(x):
    return pltpu.with_memory_space_constraint(x, pltpu.HBM)


def near(x):
    return pltpu.with_memory_space_constraint(x, pltpu.VMEM)


def body(
    tokens,
    norm_gain,
    w_filter_b,
    w_filter_c,
    w_filter_v,
    filter_taps,
    w_query,
    retention_gate_matrix,
    w_input,
    forget_gap,
    additive_fade_log,
    head_gain,
    initial_state,
    w_out_filter,
    w_out_rec,
):
    z, y, c = (lax.axis_index(a) for a in SP)
    state_rows = jnp.concatenate([retention_gate_matrix, w_input], axis=1)
    state_along_y = sent_to_all(state_rows, "sp_1").reshape(-1, state_rows.shape[1])
    rest_rows = jnp.concatenate([w_query, w_filter_b, w_filter_c, w_filter_v], axis=1)
    fade = additive_fade_log
    head = lambda a, k: lax.dynamic_slice_in_dim(a, k * HEAD_DIM, HEAD_DIM, axis=1)
    partner_fade = swapped(head(fade, 1 - c), "sp_2")
    state_along_y, rest_rows, partner_fade = lax.optimization_barrier(
        (state_along_y, rest_rows, partner_fade)
    )
    state_weights = lax.all_gather(state_along_y, ("sp_0", "sp_2"), axis=0, tiled=True)
    rest_along_y = sent_to_all(rest_rows, "sp_1").reshape(-1, rest_rows.shape[1])
    rest_weights = lax.all_gather(rest_along_y, ("sp_0", "sp_2"), axis=0, tiled=True)

    gathered = sent_to_all(tokens, "tp").reshape(-1, tokens.shape[1])
    widened = gathered.astype(f32)
    normed = (
        widened
        * lax.rsqrt(jnp.mean(widened * widened, axis=-1, keepdims=True) + epsilon)
        * norm_gain
    ).astype(bf16)
    length, width = normed.shape
    order = np.arange(256).reshape(8, 2, 16).transpose(1, 0, 2).reshape(-1)
    swap = np.zeros((256, 256), np.float32)
    swap[order, np.arange(256)] = 1.0
    own = jnp.einsum(
        "tzk,kl->tzl",
        normed.reshape(length, 8, 256),
        jnp.asarray(swap, bf16),
        preferred_element_type=f32,
    ).astype(bf16).reshape(length, width)
    partner = swapped(own, "sp_2")
    halo = shifted(own[length - HALO :], SP)

    places = jnp.stack([z, y, c])
    partner, halo, partner_fade, places = lax.optimization_barrier(
        (partner, halo, partner_fade, places)
    )

    dma = pltpu.SemaphoreType.DMA
    square = (HEAD_DIM, HEAD_DIM)
    packed_shape = jax.ShapeDtypeStruct((8, HEAD_DIM + 16, HEAD_DIM), bf16)
    packed, carried = pl.pallas_call(
        state_kernel,
        in_specs=[SMEM, VMEM, VMEM, ANY, VMEM, VMEM, ANY, ANY],
        out_specs=[VMEM] * 2,
        out_shape=[packed_shape, made((CARRIED, *square), f32)],
        scratch_shapes=[
            pltpu.VMEM((PIECES, width // PIECES, 512), bf16),
            pltpu.VMEM(square, f32),
            pltpu.VMEM(square, f32),
            dma((PIECES,)),
            dma((2,)),
        ],
        name="chip_state",
        compiler_params=granted(12),
    )(
        places,
        near(own),
        near(partner),
        far(state_weights),
        near(forget_gap[None]),
        near(fade),
        far(partner_fade),
        far(initial_state),
    )

    packed, decays, states = pl.pallas_call(
        row_kernel,
        in_specs=[SMEM] + [VMEM] * 2,
        out_specs=[VMEM] * 3,
        out_shape=[packed_shape, made((8, HEAD_DIM), f32), made((2, *square), f32)],
        name="along_row",
        compiler_params=granted(4),
    )(places, near(exchanged(packed, "sp_1")), carried)
    incoming = pl.pallas_call(
        enter_kernel,
        in_specs=[SMEM] + [VMEM] * 4,
        out_specs=VMEM,
        out_shape=made((2, *square), bf16),
        name="enter_chip",
        compiler_params=granted(4),
    )(places, near(exchanged(packed, "sp_0")), carried, decays, states)
    incoming = exchanged(incoming, "sp_2")

    partial = pl.pallas_call(
        final_kernel,
        in_specs=[ANY, ANY, ANY] + [VMEM] * 5 + [ANY],
        out_specs=VMEM,
        out_shape=made((length, width), bf16),
        scratch_shapes=[
            pltpu.VMEM((PIECES, width // PIECES, 1024), bf16),
            pltpu.VMEM((HALO + length, width), bf16),
            pltpu.VMEM((256, width), bf16),
            dma((PIECES,)),
            dma((2,)),
            dma((1,)),
        ],
        name="outputs",
        compiler_params=granted(20),
    )(
        far(halo),
        far(own),
        far(rest_weights),
        carried,
        near(filter_taps),
        near(incoming),
        near(head_gain[None]),
        near(w_out_filter),
        far(w_out_rec),
    )
    arrived = exchanged(partial.reshape(4, length // 4, -1), "tp")
    return arrived.astype(f32).sum(axis=0).astype(bf16)


def solution(mesh):
    torus = Mesh(mesh.devices.reshape(8, 8, 2, mesh.shape["tp"]), ("sp_0", "sp_1", "sp_2", "tp"))
    placed = (
        P(SP_TP, None),
        P(),
        P(SP, "tp"),
        P(SP, "tp"),
        P(SP, "tp"),
        P(None, "tp"),
        P(SP, "tp"),
        P(SP, "tp"),
        P(SP, "tp"),
        P("tp"),
        P(SP, "tp"),
        P(),
        P("tp", None, None),
        P("tp", None),
        P("tp", None),
    )
    return jax.shard_map(
        body, mesh=torus, in_specs=placed, out_specs=P(SP_TP, None), check_vma=False
    )
```
